512 devices in a mesh: rep: 64 (over z, y), fs: 4 (over x), tp: 2 (over core).
Axes of the slice: x: 4, y: 8, z: 8, core: 2. Of those that a mesh axis runs over, the one named last changes fastest.
Arguments:
- pre_act: bfloat16 [65536, 4096], P('rep', ('fs', 'tp')), may hold values from -6 to 6
- down_weight: bfloat16 [4096, 2048], P(('fs', 'tp')), may hold values from -0.09375 to 0.09375
- cotangent: bfloat16 [65536, 2048], P('rep', ('fs', 'tp')), may hold values from -16 to 16
Outputs:
- grad_pre: bfloat16 [65536, 4096], P('rep', ('fs', 'tp'))
- grad_weight: float32 [4096, 2048], P(('fs', 'tp', 'rep'))
The draws below stay inside these ranges and needn't reach their ends.
All inputs are finite; a program needn't handle non-finite values.
Results may differ from the reference program's by a relative error of at most 0.0029.
Values may be sent and summed in bfloat16 or wider, within the bound.
No kernel may reach another device: no remote copies, remote signals or barrier semaphores. Data moves between devices by JAX's collectives and lax.ppermute only.
A program may use at most 64 MiB of HBM per device.

```python
import jax
import jax.numpy as jnp

D = 2048
FF = 4096
TOKENS = 65536


def with_spikes(array, own_key, source, target, parts, factor):
    def block_of(position):
        return (jnp.arange(array.shape[position]) // (array.shape[position] // parts)).reshape((-1,) + (1,) * (array.ndim - 1 - position))

    first = jax.random.permutation(own_key, parts)[block_of(target)]
    other_side = (block_of(target) + parts // 2) % parts
    return jnp.where((block_of(source) == first) | (block_of(source) == other_side), factor * array, array)


def level_of(rng, dims, split, smallest, largest):
    factor_of = 1.0
    for axis_at, blocks in split:
        draws = jax.random.uniform(jax.random.fold_in(jax.random.fold_in(rng, 6), axis_at), (blocks,), jnp.float32, smallest / len(split), largest / len(split))
        factor_of = factor_of * jnp.repeat(jnp.exp(draws), dims[axis_at] // blocks).reshape((-1,) + (1,) * (len(dims) - 1 - axis_at))
    return factor_of


def bell_draw(key, extent, deviation, bound, cuts=(), kind=jnp.bfloat16):
    factor_of = level_of(key, extent, cuts, -0.22, 0.18) if cuts else 1.0
    drawn = jax.random.normal(key, extent, jnp.float32) * deviation * factor_of
    return jnp.minimum(jnp.maximum(drawn, -bound), bound).astype(kind)


def bell_draw_with(stream_key, dims, deviation, most, split, heavy, kind=jnp.bfloat16):
    entries = deviation * jax.random.normal(stream_key, dims, jnp.float32)
    if split:
        entries = entries * level_of(stream_key, dims, split, -0.22, 0.18)
    return jnp.clip(with_spikes(entries, jax.random.fold_in(stream_key, 3), *heavy), -most, most).astype(kind)


def setup_inputs(seed: int = 0) -> dict:
    arg_keys = jax.random.split(jax.random.key(seed), 4)
    pre_act = bell_draw(arg_keys[0], (TOKENS, FF), 1.0, 6.0, ((0, 64), (1, 8)))
    down_weight = bell_draw(arg_keys[1], (FF, D), FF ** -0.5, 0.09375, ((0, 8),))
    cotangent = bell_draw_with(arg_keys[2], (TOKENS, D), 1.0, 16.0, ((0, 64), (1, 8)), (0, 1, 64, 4.0))
    return {"pre_act": pre_act, "down_weight": down_weight, "cotangent": cotangent}


def reference(pre_act, down_weight, cotangent):
    grad_hidden = jnp.dot(cotangent, down_weight.T, preferred_element_type=jnp.float32)
    positive = jnp.maximum(pre_act.astype(jnp.float32), 0.0)
    grad_pre = (grad_hidden * 2.0 * positive).astype(jnp.bfloat16)
    hidden = (positive * positive).astype(jnp.bfloat16)
    summed = jnp.dot(hidden.T, cotangent, preferred_element_type=jnp.float32)
    grad_weight = summed * (1.0 / jnp.sqrt(jnp.float32(TOKENS)))
    return (grad_pre, grad_weight)
```

```python
import math

import jax
import jax.numpy as jnp
import numpy as np
from jax import lax
from jax.experimental import pallas as pl
from jax.experimental.pallas import tpu as pltpu
from jax.sharding import Mesh
from jax.sharding import PartitionSpec as P

REP = ("z", "y")
COL = ("fs", "tp")
GROUP = ("z", "y", "tp")
BF16 = jnp.bfloat16
F32 = jnp.float32


def lines(size):
    index = np.arange(size * size * 2).reshape(size, size, 2)
    return np.concatenate([index[..., 0].T, index[..., 1]]).tolist()


def other_lines(size):
    index = np.arange(size * size * 2).reshape(size, size, 2)
    return np.concatenate([index[..., 0], index[..., 1].T]).tolist()


def swap(rows, groups):
    parts = len(groups[0])
    got = lax.all_to_all(rows, GROUP, 0, 0, axis_index_groups=groups, tiled=True)
    return got.reshape(parts, rows.shape[0] // parts, rows.shape[1])


def other_core(x):
    return lax.ppermute(x, "tp", [(0, 1), (1, 0)])


def along(x, by):
    n = lax.axis_size("fs")
    pairs = [(2 * i + c, 2 * ((i + (by, -by)[c]) % n) + c) for i in range(n) for c in range(2)]
    return lax.ppermute(x, COL, pairs)


def piece(n, position):
    core = position % 2
    ahead = 2 * core - 1
    chip = (position // 2 + 4 + (0, 0, ahead, -ahead, -ahead, ahead, 2, 2)[n]) % 4
    return chip * 2 + (core + n) % 2


def hidden_kernel(at_ref, pre_ref, out_ref):
    units = pre_ref.shape[1]
    target = lax.broadcasted_iota(jnp.int32, (units, 1), 0)
    turned = target // 8 % 8 * 64 + target // 64 * 8 + target % 8
    source = jnp.where(at_ref[0] % 2 == 0, target, turned)
    pick = (lax.broadcasted_iota(jnp.int32, (units, units), 1) == source).astype(F32).astype(BF16)
    positive = jnp.maximum(pre_ref[...].astype(F32), 0.0)
    hidden = (positive * positive).astype(BF16)
    out_ref[...] = lax.dot_general(
        pick, hidden, (((1,), (1,)), ((), ())), preferred_element_type=F32
    ).astype(BF16)


def hidden_of(at, pre_act):
    tokens, units = pre_act.shape
    block = tokens // 2
    return pl.pallas_call(
        hidden_kernel,
        out_shape=jax.ShapeDtypeStruct((units, tokens), BF16),
        grid=(2,),
        in_specs=[
            pl.BlockSpec(memory_space=pltpu.SMEM),
            pl.BlockSpec((block, units), lambda i: (i, 0)),
        ],
        out_specs=pl.BlockSpec((units, block), lambda i: (0, i)),
        cost_estimate=pl.CostEstimate(
            flops=2 * units * units * tokens, bytes_accessed=4 * units * tokens, transcendentals=0
        ),
        name="hidden",
    )(at, pre_act)


def term_kernel(count, hidden_ref, *refs):
    out_ref = refs[-1]
    width = refs[0].shape[1]
    for n in range(count):
        out_ref[:, n * width : (n + 1) * width] = jnp.dot(
            hidden_ref[...], refs[n][...], preferred_element_type=F32
        ).astype(BF16)


def term_of(hidden, pieces, first, total, base=None):
    units, tokens = hidden.shape
    width = pieces[0].shape[1]
    count, steps = len(pieces), 2
    whole = pl.BlockSpec((tokens, width), lambda i: (0, 0))
    extra = () if base is None else (base,)
    return pl.pallas_call(
        lambda *refs: term_kernel(count, *refs),
        out_shape=jax.ShapeDtypeStruct((units, width * total), BF16),
        grid=(steps,),
        in_specs=[pl.BlockSpec((units // steps, tokens), lambda i: (i, 0))]
        + [whole] * count
        + [pl.BlockSpec(memory_space=pl.ANY)] * len(extra),
        out_specs=pl.BlockSpec((units // steps, width * count), lambda i: (i, first // count)),
        input_output_aliases={1 + count: 0} if extra else {},
        cost_estimate=pl.CostEstimate(
            flops=2 * units * tokens * width * count,
            bytes_accessed=2 * (units * tokens + width * count * (tokens + units)),
            transcendentals=0,
        ),
        name="term",
    )(hidden, *pieces, *extra)


def grad_pre_kernel(at_ref, pre_ref, weight_ref, *refs):
    parts, out_ref = refs[:-1], refs[-1]
    width = parts[0].shape[1]
    total = jnp.zeros(out_ref.shape, F32)
    for n, part in enumerate(parts):
        columns = pl.ds(pl.multiple_of(piece(n, at_ref[0]) * width, width), width)
        total += lax.dot_general(
            part[...], weight_ref[:, columns], (((1,), (1,)), ((), ())), preferred_element_type=F32
        )
    positive = jnp.maximum(pre_ref[...].astype(F32), 0.0)
    out_ref[...] = (total * 2.0 * positive).astype(BF16)


def grad_pre_of(at, pre_act, down_weight, parts):
    tokens, units = pre_act.shape
    block = tokens // 4
    width = parts[0].shape[1]
    return pl.pallas_call(
        grad_pre_kernel,
        out_shape=jax.ShapeDtypeStruct((tokens, units), BF16),
        grid=(4,),
        in_specs=[
            pl.BlockSpec(memory_space=pltpu.SMEM),
            pl.BlockSpec((block, units), lambda i: (i, 0)),
            pl.BlockSpec(down_weight.shape, lambda i: (0, 0)),
        ]
        + [pl.BlockSpec((block, width), lambda i: (i, 0))] * len(parts),
        out_specs=pl.BlockSpec((block, units), lambda i: (i, 0)),
        cost_estimate=pl.CostEstimate(
            flops=2 * tokens * units * width * len(parts),
            bytes_accessed=2 * (2 * tokens * units + down_weight.size + tokens * width * len(parts)),
            transcendentals=0,
        ),
        name="grad_pre",
    )(at, pre_act, down_weight, *parts)


def place_kernel(factor, width, at_ref, got_ref, out_ref):
    for n in range(out_ref.shape[1] // width):
        columns = slice(n * width, (n + 1) * width)
        total = got_ref[0, :, columns].astype(F32)
        for k in range(1, got_ref.shape[0]):
            total += got_ref[k, :, columns].astype(F32)
        target = pl.ds(pl.multiple_of(piece(n, at_ref[0]) * width, width), width)
        out_ref[:, target] = total * factor


def place(at, got, factor, width):
    return pl.pallas_call(
        lambda *refs: place_kernel(factor, width, *refs),
        out_shape=jax.ShapeDtypeStruct(got.shape[1:], F32),
        in_specs=[
            pl.BlockSpec(memory_space=pltpu.SMEM),
            pl.BlockSpec(memory_space=pltpu.VMEM),
        ],
        out_specs=pl.BlockSpec(memory_space=pltpu.VMEM),
        cost_estimate=pl.CostEstimate(
            flops=got.size, bytes_accessed=4 * got.size, transcendentals=0
        ),
        name="place",
    )(at, got)


def step(pre_act, down_weight, cotangent):
    tokens, width = cotangent.shape
    size = lax.axis_size("z")
    at = lax.axis_index(COL).astype(jnp.int32).reshape(1)

    one = along(cotangent, 1)
    own = other_core(cotangent)
    two = along(cotangent, -1)
    three = along(one, 1)
    pieces = (cotangent, own, one, other_core(one))
    pieces += (two, other_core(two), three, other_core(three))

    hidden = hidden_of(at, pre_act)
    term = term_of(hidden, pieces[:6], 0, 8)
    term = term_of(hidden, pieces[6:], 6, 8, term)
    got = swap(term, lines(size))
    joined = jnp.sum(got.astype(F32), axis=0).astype(BF16)
    got = swap(joined, other_lines(size))

    factor = 1.0 / math.sqrt(tokens * size * size)
    grad_weight = place(at, got, factor, width)
    grad_pre = grad_pre_of(at, pre_act, down_weight, pieces)
    return (grad_pre, grad_weight)


def solution(mesh):
    finer = Mesh(
        mesh.devices.reshape(8, 8, mesh.shape["fs"], mesh.shape["tp"]),
        REP + COL,
    )
    in_specs = (P(REP, COL), P(COL, None), P(REP, COL))
    out_specs = (P(REP, COL), P(COL + REP, None))
    return jax.shard_map(step, mesh=finer, in_specs=in_specs, out_specs=out_specs, check_vma=False)
```

```python
import math

import jax
import jax.numpy as jnp
import numpy as np
from jax import lax
from jax.experimental import pallas as pl
from jax.experimental.pallas import tpu as pltpu
from jax.sharding import Mesh
from jax.sharding import PartitionSpec as P

REP = ("z", "y")
COL = ("fs", "tp")
GROUP = ("z", "y", "tp")
BF16 = jnp.bfloat16
F32 = jnp.float32
VMEM = pl.BlockSpec(memory_space=pltpu.VMEM)
SMALL = pltpu.CompilerParams(vmem_limit_bytes=16 * 2**20)


def lines(size):
    index = np.arange(size * size * 2).reshape(size, size, 2)
    return np.concatenate([index[..., 0].T, index[..., 1]]).tolist()


def other_lines(size):
    index = np.arange(size * size * 2).reshape(size, size, 2)
    return np.concatenate([index[..., 0], index[..., 1].T]).tolist()


def swap(rows, groups):
    parts = len(groups[0])
    got = lax.all_to_all(rows, GROUP, 0, 0, axis_index_groups=groups, tiled=True)
    return got.reshape(parts, rows.shape[0] // parts, rows.shape[1])


def other_core(x):
    return lax.ppermute(x, "tp", [(0, 1), (1, 0)])


def along(x, by):
    n = lax.axis_size("fs")
    pairs = [(2 * i + c, 2 * ((i + (by, -by)[c]) % n) + c) for i in range(n) for c in range(2)]
    return lax.ppermute(x, COL, pairs)


def piece(n, position):
    core = position % 2
    ahead = 2 * core - 1
    chip = (position // 2 + 4 + (0, 0, ahead, -ahead, -ahead, ahead, 2, 2)[n]) % 4
    return chip * 2 + (core + n) % 2


def hidden_kernel(at_ref, pre_ref, out_ref):
    units = pre_ref.shape[1]
    target = lax.broadcasted_iota(jnp.int32, (units, 1), 0)
    turned = target // 8 % 8 * 64 + target // 64 * 8 + target % 8
    source = jnp.where(at_ref[0] % 2 == 0, target, turned)
    pick = (lax.broadcasted_iota(jnp.int32, (units, units), 1) == source).astype(F32).astype(BF16)
    positive = jnp.maximum(pre_ref[...].astype(F32), 0.0)
    hidden = (positive * positive).astype(BF16)
    out_ref[...] = lax.dot_general(
        pick, hidden, (((1,), (1,)), ((), ())), preferred_element_type=F32
    ).astype(BF16)


def hidden_of(at, pre_act):
    tokens, units = pre_act.shape
    block = tokens // 2
    return pl.pallas_call(
        hidden_kernel,
        out_shape=jax.ShapeDtypeStruct((units, tokens), BF16),
        grid=(2,),
        in_specs=[
            pl.BlockSpec(memory_space=pltpu.SMEM),
            pl.BlockSpec((block, units), lambda i: (i, 0)),
        ],
        out_specs=pl.BlockSpec((units, block), lambda i: (0, i)),
        cost_estimate=pl.CostEstimate(
            flops=2 * units * units * tokens, bytes_accessed=4 * units * tokens, transcendentals=0
        ),
        compiler_params=SMALL,
        name="hidden",
    )(at, pre_act)


def term_kernel(count, hidden_ref, *refs):
    out_ref = refs[-1]
    width = refs[0].shape[1]
    for n in range(count):
        out_ref[:, n * width : (n + 1) * width] = jnp.dot(
            hidden_ref[...], refs[n][...], preferred_element_type=F32
        ).astype(BF16)


def term_of(hidden, pieces, first, total, base=None):
    units, tokens = hidden.shape
    width = pieces[0].shape[1]
    count = len(pieces)
    extra = () if base is None else (base,)
    return pl.pallas_call(
        lambda *refs: term_kernel(count, *refs),
        out_shape=jax.ShapeDtypeStruct((units, width * total), BF16),
        grid=(1,),
        in_specs=[VMEM] * (1 + count) + [pl.BlockSpec(memory_space=pl.ANY)] * len(extra),
        out_specs=pl.BlockSpec((units, width * count), lambda i: (0, first // count)),
        input_output_aliases={1 + count: 0} if extra else {},
        compiler_params=SMALL,
        cost_estimate=pl.CostEstimate(
            flops=2 * units * tokens * width * count,
            bytes_accessed=2 * (units * tokens + width * count * (tokens + units)),
            transcendentals=0,
        ),
        name="term",
    )(hidden, *pieces, *extra)


def grad_pre_kernel(at_ref, pre_ref, weight_ref, *refs):
    parts, out_ref = refs[:-1], refs[-1]
    width = parts[0].shape[1]
    total = jnp.zeros(out_ref.shape, F32)
    for n, part in enumerate(parts):
        columns = pl.ds(pl.multiple_of(piece(n, at_ref[0]) * width, width), width)
        total += lax.dot_general(
            part[...], weight_ref[:, columns], (((1,), (1,)), ((), ())), preferred_element_type=F32
        )
    positive = jnp.maximum(pre_ref[...].astype(F32), 0.0)
    out_ref[...] = (total * 2.0 * positive).astype(BF16)


def grad_pre_of(at, pre_act, down_weight, parts):
    tokens, units = pre_act.shape
    block = tokens // 4
    width = parts[0].shape[1]
    return pl.pallas_call(
        grad_pre_kernel,
        out_shape=jax.ShapeDtypeStruct((tokens, units), BF16),
        grid=(4,),
        in_specs=[
            pl.BlockSpec(memory_space=pltpu.SMEM),
            pl.BlockSpec((block, units), lambda i: (i, 0)),
            pl.BlockSpec(down_weight.shape, lambda i: (0, 0)),
        ]
        + [pl.BlockSpec((block, width), lambda i: (i, 0))] * len(parts),
        out_specs=pl.BlockSpec((block, units), lambda i: (i, 0)),
        cost_estimate=pl.CostEstimate(
            flops=2 * tokens * units * width * len(parts),
            bytes_accessed=2 * (2 * tokens * units + down_weight.size + tokens * width * len(parts)),
            transcendentals=0,
        ),
        name="grad_pre",
    )(at, pre_act, down_weight, *parts)


def place_kernel(factor, width, at_ref, got_ref, out_ref):
    for n in range(out_ref.shape[1] // width):
        columns = slice(n * width, (n + 1) * width)
        total = got_ref[0, :, columns].astype(F32)
        for k in range(1, got_ref.shape[0]):
            total += got_ref[k, :, columns].astype(F32)
        target = pl.ds(pl.multiple_of(piece(n, at_ref[0]) * width, width), width)
        out_ref[:, target] = total * factor


def place(at, got, factor, width):
    return pl.pallas_call(
        lambda *refs: place_kernel(factor, width, *refs),
        out_shape=jax.ShapeDtypeStruct(got.shape[1:], F32),
        in_specs=[
            pl.BlockSpec(memory_space=pltpu.SMEM),
            pl.BlockSpec(memory_space=pltpu.VMEM),
        ],
        out_specs=pl.BlockSpec(memory_space=pltpu.VMEM),
        cost_estimate=pl.CostEstimate(
            flops=got.size, bytes_accessed=4 * got.size, transcendentals=0
        ),
        compiler_params=SMALL,
        name="place",
    )(at, got)


def step(pre_act, down_weight, cotangent):
    tokens, width = cotangent.shape
    size = lax.axis_size("z")
    at = lax.axis_index(COL).astype(jnp.int32).reshape(1)

    one = along(cotangent, 1)
    own = other_core(cotangent)
    two = along(cotangent, -1)
    three = along(one, 1)
    pieces = (cotangent, own, one, other_core(one))
    pieces += (two, other_core(two), three, other_core(three))

    hidden = hidden_of(at, pre_act)
    term = term_of(hidden, pieces[:4], 0, 8)
    term = term_of(hidden, pieces[4:], 4, 8, term)
    got = swap(term, lines(size))
    joined = jnp.sum(got.astype(F32), axis=0).astype(BF16)
    got = swap(joined, other_lines(size))

    factor = 1.0 / math.sqrt(tokens * size * size)
    grad_weight = place(at, got, factor, width)
    grad_pre = grad_pre_of(at, pre_act, down_weight, pieces)
    return (grad_pre, grad_weight)


def solution(mesh):
    finer = Mesh(
        mesh.devices.reshape(8, 8, mesh.shape["fs"], mesh.shape["tp"]),
        REP + COL,
    )
    in_specs = (P(REP, COL), P(COL, None), P(REP, COL))
    out_specs = (P(REP, COL), P(COL + REP, None))
    return jax.shard_map(step, mesh=finer, in_specs=in_specs, out_specs=out_specs, check_vma=False)
```

```python
import math

import jax
import jax.numpy as jnp
import numpy as np
from jax import lax
from jax.experimental import pallas as pl
from jax.experimental.pallas import tpu as pltpu
from jax.sharding import Mesh
from jax.sharding import PartitionSpec as P

REP = ("z", "y")
COL = ("fs", "tp")
GROUP = ("z", "y", "tp")
BF16 = jnp.bfloat16
F32 = jnp.float32
VMEM = pl.BlockSpec(memory_space=pltpu.VMEM)
SMALL = pltpu.CompilerParams(vmem_limit_bytes=16 * 2**20)


def lines(size):
    index = np.arange(size * size * 2).reshape(size, size, 2)
    return np.concatenate([index[..., 0].T, index[..., 1]]).tolist()


def other_lines(size):
    index = np.arange(size * size * 2).reshape(size, size, 2)
    return np.concatenate([index[..., 0], index[..., 1].T]).tolist()


def swap(rows, groups):
    parts = len(groups[0])
    got = lax.all_to_all(rows, GROUP, 0, 0, axis_index_groups=groups, tiled=True)
    return got.reshape(parts, rows.shape[0] // parts, rows.shape[1])


def other_core(x):
    return lax.ppermute(x, "tp", [(0, 1), (1, 0)])


def along(x, by):
    n = lax.axis_size("fs")
    pairs = [(2 * i + c, 2 * ((i + (by, -by)[c]) % n) + c) for i in range(n) for c in range(2)]
    return lax.ppermute(x, COL, pairs)


def piece(n, position):
    core = position % 2
    ahead = 2 * core - 1
    chip = (position // 2 + 4 + (0, 0, ahead, -ahead, -ahead, ahead, 2, 2)[n]) % 4
    return chip * 2 + (core + n) % 2


def hidden_kernel(at_ref, pre_ref, out_ref):
    units = pre_ref.shape[1]
    target = lax.broadcasted_iota(jnp.int32, (units, 1), 0)
    turned = target // 8 % 8 * 64 + target // 64 * 8 + target % 8
    source = jnp.where(at_ref[0] % 2 == 0, target, turned)
    pick = (lax.broadcasted_iota(jnp.int32, (units, units), 1) == source).astype(F32).astype(BF16)
    positive = jnp.maximum(pre_ref[...].astype(F32), 0.0)
    hidden = (positive * positive).astype(BF16)
    out_ref[...] = lax.dot_general(
        pick, hidden, (((1,), (1,)), ((), ())), preferred_element_type=F32
    ).astype(BF16)


def hidden_of(at, pre_act):
    tokens, units = pre_act.shape
    block = tokens // 2
    return pl.pallas_call(
        hidden_kernel,
        out_shape=jax.ShapeDtypeStruct((units, tokens), BF16),
        grid=(2,),
        in_specs=[
            pl.BlockSpec(memory_space=pltpu.SMEM),
            pl.BlockSpec((block, units), lambda i: (i, 0)),
        ],
        out_specs=pl.BlockSpec((units, block), lambda i: (0, i)),
        cost_estimate=pl.CostEstimate(
            flops=2 * units * units * tokens, bytes_accessed=4 * units * tokens, transcendentals=0
        ),
        compiler_params=SMALL,
        name="hidden",
    )(at, pre_act)


def term_kernel(count, hidden_ref, *refs):
    out_ref = refs[-1]
    width = refs[0].shape[1]
    for n in range(count):
        out_ref[:, n * width : (n + 1) * width] = jnp.dot(
            hidden_ref[...], refs[n][...], preferred_element_type=F32
        ).astype(BF16)


def term_of(hidden, pieces, first, total, base=None):
    units, tokens = hidden.shape
    width = pieces[0].shape[1]
    count = len(pieces)
    extra = () if base is None else (base,)
    return pl.pallas_call(
        lambda *refs: term_kernel(count, *refs),
        out_shape=jax.ShapeDtypeStruct((units, width * total), BF16),
        grid=(1,),
        in_specs=[VMEM] * (1 + count) + [pl.BlockSpec(memory_space=pl.ANY)] * len(extra),
        out_specs=pl.BlockSpec((units, width * count), lambda i: (0, first // count)),
        input_output_aliases={1 + count: 0} if extra else {},
        compiler_params=SMALL,
        cost_estimate=pl.CostEstimate(
            flops=2 * units * tokens * width * count,
            bytes_accessed=2 * (units * tokens + width * count * (tokens + units)),
            transcendentals=0,
        ),
        name="term",
    )(hidden, *pieces, *extra)


def grad_pre_kernel(at_ref, pre_ref, weight_ref, *refs):
    parts, out_ref = refs[:-1], refs[-1]
    width = parts[0].shape[1]
    total = jnp.zeros(out_ref.shape, F32)
    for n, part in enumerate(parts):
        columns = pl.ds(pl.multiple_of(piece(n, at_ref[0]) * width, width), width)
        total += lax.dot_general(
            part[...], weight_ref[:, columns], (((1,), (1,)), ((), ())), preferred_element_type=F32
        )
    positive = jnp.maximum(pre_ref[...].astype(F32), 0.0)
    out_ref[...] = (total * 2.0 * positive).astype(BF16)


def grad_pre_of(at, pre_act, down_weight, parts):
    tokens, units = pre_act.shape
    block = tokens // 4
    width = parts[0].shape[1]
    return pl.pallas_call(
        grad_pre_kernel,
        out_shape=jax.ShapeDtypeStruct((tokens, units), BF16),
        grid=(4,),
        in_specs=[
            pl.BlockSpec(memory_space=pltpu.SMEM),
            pl.BlockSpec((block, units), lambda i: (i, 0)),
            pl.BlockSpec(down_weight.shape, lambda i: (0, 0)),
        ]
        + [pl.BlockSpec((block, width), lambda i: (i, 0))] * len(parts),
        out_specs=pl.BlockSpec((block, units), lambda i: (i, 0)),
        cost_estimate=pl.CostEstimate(
            flops=2 * tokens * units * width * len(parts),
            bytes_accessed=2 * (2 * tokens * units + down_weight.size + tokens * width * len(parts)),
            transcendentals=0,
        ),
        name="grad_pre",
    )(at, pre_act, down_weight, *parts)


def place_kernel(factor, width, at_ref, got_ref, out_ref):
    for n in range(out_ref.shape[1] // width):
        columns = slice(n * width, (n + 1) * width)
        total = got_ref[0, :, columns].astype(F32)
        for k in range(1, got_ref.shape[0]):
            total += got_ref[k, :, columns].astype(F32)
        target = pl.ds(pl.multiple_of(piece(n, at_ref[0]) * width, width), width)
        out_ref[:, target] = total * factor


def place(at, got, factor, width):
    return pl.pallas_call(
        lambda *refs: place_kernel(factor, width, *refs),
        out_shape=jax.ShapeDtypeStruct(got.shape[1:], F32),
        in_specs=[
            pl.BlockSpec(memory_space=pltpu.SMEM),
            pl.BlockSpec(memory_space=pltpu.VMEM),
        ],
        out_specs=pl.BlockSpec(memory_space=pltpu.VMEM),
        cost_estimate=pl.CostEstimate(
            flops=got.size, bytes_accessed=4 * got.size, transcendentals=0
        ),
        compiler_params=SMALL,
        name="place",
    )(at, got)


def step(pre_act, down_weight, cotangent):
    tokens, width = cotangent.shape
    size = lax.axis_size("z")
    at = lax.axis_index(COL).astype(jnp.int32).reshape(1)

    one = along(cotangent, 1)
    own = other_core(cotangent)
    two = along(cotangent, -1)
    three = along(one, 1)
    pieces = (cotangent, own, one, other_core(one))
    pieces += (two, other_core(two), three, other_core(three))

    hidden = hidden_of(at, pre_act)
    term = term_of(hidden, pieces[:2], 0, 8)
    term = term_of(hidden, pieces[2:4], 2, 8, term)
    term = term_of(hidden, pieces[4:6], 4, 8, term)
    term = term_of(hidden, pieces[6:], 6, 8, term)
    got = swap(term, lines(size))
    joined = jnp.sum(got.astype(F32), axis=0).astype(BF16)
    got = swap(joined, other_lines(size))

    factor = 1.0 / math.sqrt(tokens * size * size)
    grad_weight = place(at, got, factor, width)
    grad_pre = grad_pre_of(at, pre_act, down_weight, pieces)
    return (grad_pre, grad_weight)


def solution(mesh):
    finer = Mesh(
        mesh.devices.reshape(8, 8, mesh.shape["fs"], mesh.shape["tp"]),
        REP + COL,
    )
    in_specs = (P(REP, COL), P(COL, None), P(REP, COL))
    out_specs = (P(REP, COL), P(COL + REP, None))
    return jax.shard_map(step, mesh=finer, in_specs=in_specs, out_specs=out_specs, check_vma=False)
```
